32 devices in a mesh: kv: 8 (over z, y), tp: 4 (over x, core).
Axes of the slice: x: 2, y: 2, z: 4, core: 2. Of those that a mesh axis runs over, the one named last changes fastest.
Arguments:
- tokens: bfloat16 [16, 4096], P(None, 'kv'), may hold values from -6 to 6
- norm_gain: float32 [4096], P('kv'), may hold values from 0.1 to 1.9
- query_weight: bfloat16 [4096, 2048], P('kv', 'tp'), may hold values from -1 to 1
- key_weight: bfloat16 [4096, 2048], P('kv', 'tp'), may hold values from -0.09375 to 0.09375
- value_weight: bfloat16 [4096, 2048], P('kv', 'tp'), may hold values from -0.09375 to 0.09375
- out_weight: bfloat16 [2048, 4096], P('tp', 'kv'), may hold values from -0.125 to 0.125
- lambdas: float32 [16], P('tp'), may hold values from 0.3 to 0.8
- head_gain: float32 [128], replicated, may hold values from 0.1 to 1.9
- lengths: int32 [16], replicated, may hold values from 1 to 8191, as said below
- key_cache: bfloat16 [16, 8192, 16, 128], P(None, 'kv', 'tp'), may hold values from -48 to 48, as said below
- value_cache: bfloat16 [16, 8192, 16, 128], P(None, 'kv', 'tp'), may hold values from -6 to 6
Outputs:
- attended: bfloat16 [16, 4096], P(None, 'kv')
The draws below stay inside these ranges and needn't reach their ends.
Inputs may be any that keep to these rules, and one draw needn't show every extreme that they name: `lengths`: each sequence has 1 to 8191 cached tokens. `key_cache`: cached keys lie between -48 and 48.
All inputs are finite; a program needn't handle non-finite values.
Results may differ from the reference program's by a relative error of at most 0.012.
The reference program's roundings to bfloat16 on the way (of `normed`, `fresh_value`, `weights` and `head_out`) count: a program that leaves them out, or rounds other values in their place, can miss the bound.
Values may be sent and summed in bfloat16 or wider, within the bound.
A program may use at most 128 MiB of HBM per device.

```python
import jax
import jax.numpy as jnp
from jax import lax

D = 4096
H = 16
DH = 64
SEQS = 16
POS_DEV = 1024
CACHE_LEN = 8192
N_KV = 8


def token_values(key):
    base = jax.random.fold_in(key, 11)
    drawn = jnp.clip(jax.random.normal(base, (SEQS, D), jnp.float32), -6.0, 6.0)
    return drawn.astype(jnp.bfloat16)


def gain_values(key):
    base = jax.random.fold_in(key, 12)
    drawn = 1.0 + 0.18 * jnp.clip(jax.random.normal(base, (D,), jnp.float32), -5.0, 5.0)
    return drawn


def weight_values(key):
    base = jax.random.fold_in(key, 13)
    whole_shape = (D, H * 2 * DH)
    drawn = jnp.clip(jax.random.normal(base, whole_shape, jnp.float32), -6.0, 6.0)
    return (drawn * D ** (-0.5)).astype(jnp.bfloat16)


def length_values(key):
    base = jax.random.fold_in(key, 14)
    return jax.random.randint(base, (SEQS,), 1, CACHE_LEN).astype(jnp.int32)


def draw_tokens(key, part):
    return token_values(key)


def draw_norm_gain(key, part):
    return gain_values(key)


def draw_query_weight(key, part):
    return weight_values(key)


def draw_lengths(key, part):
    return length_values(key)


def draw_key_cache(key, part):
    base = jax.random.fold_in(key, 15)
    whole_shape = (SEQS, CACHE_LEN, H, 2 * DH)
    drawn = jnp.clip(1.5 * jax.random.normal(base, whole_shape, jnp.float32), -9.0, 9.0)
    return drawn.astype(jnp.bfloat16)


def levels(rng, shape, cuts, low, largest):
    factor_of, own = 1.0, jax.random.fold_in(rng, 6)
    for dim, shards_of in cuts:
        heights = jnp.exp(jax.random.uniform(jax.random.fold_in(own, dim), (shards_of,), jnp.float32, low / len(cuts), largest / len(cuts)))
        factor_of = factor_of * jnp.repeat(heights, shape[dim] // shards_of).reshape([-1 if axis == dim else 1 for axis in range(len(shape))])
    return factor_of


def centred(stream_key, shape, deviation, reach, pieces=(), kind=jnp.bfloat16):
    gain = levels(stream_key, shape, pieces, -0.22, 0.18) if pieces else 1.0
    entries = jax.random.normal(stream_key, shape, jnp.float32) * deviation * gain
    return jnp.minimum(jnp.maximum(entries, -reach), reach).astype(kind)


def setup_inputs(seed: int = 0) -> dict:
    splits = jax.random.split(jax.random.key(seed), 12)
    tokens = draw_tokens(jax.random.fold_in(splits[11], 71), 0)
    norm_gain = draw_norm_gain(jax.random.fold_in(splits[11], 71), 0)
    query_weight = draw_query_weight(jax.random.fold_in(splits[11], 71), 0)
    key_weight = centred(splits[3], (D, H * 2 * DH), D ** -0.5, 0.09375, ((0, 8), (1, 4)))
    value_weight = centred(splits[4], (D, H * 2 * DH), D ** -0.5, 0.09375, ((0, 8), (1, 4)))
    out_weight = centred(splits[5], (H * 2 * DH, D), (H * 2 * DH) ** -0.5, 0.125, ((0, 4), (1, 8)))
    lambdas = jnp.clip(0.3 + 0.5 * jax.random.uniform(splits[6], (H,), jnp.float32) ** levels(splits[6], (H,), ((0, 4),), -0.2, 0.2), 0.3, 0.8)
    head_gain = jnp.clip(1.0 + 0.18 * jax.random.normal(splits[7], (2 * DH,), jnp.float32), 0.1, 1.9)
    lengths = draw_lengths(jax.random.fold_in(splits[11], 71), 0)
    key_cache = draw_key_cache(jax.random.fold_in(splits[11], 71), 0)
    value_cache = centred(splits[10], (SEQS, CACHE_LEN, H, 2 * DH), 1.0, 6.0, ((1, 8), (2, 4)))
    return {"tokens": tokens, "norm_gain": norm_gain, "query_weight": query_weight, "key_weight": key_weight, "value_weight": value_weight, "out_weight": out_weight, "lambdas": lambdas, "head_gain": head_gain, "lengths": lengths, "key_cache": key_cache, "value_cache": value_cache}


epsilon = 1e-05
theta_base = 500000.0
floor_value = -1e+30

def angles_for(positions, width):
    halfway = width // 2
    frequency = theta_base ** (-jnp.arange(halfway, dtype=jnp.float32) / halfway)
    return positions.astype(jnp.float32)[:, None] * frequency[None, :]

def rotate(values_in, angles):
    halfway = values_in.shape[-1] // 2
    cosine = jnp.cos(angles)[:, None, None, :]
    sine_part = jnp.sin(angles)[:, None, None, :]
    former = values_in[..., :halfway]
    latter = values_in[..., halfway:]
    return jnp.concatenate([former * cosine - latter * sine_part, latter * cosine + former * sine_part], axis=-1)

def reference(tokens, norm_gain, query_weight, key_weight, value_weight, out_weight, lambdas, head_gain, lengths, key_cache, value_cache):
    widened = tokens.astype(jnp.float32)
    row_scale = lax.rsqrt(lax.optimization_barrier(jnp.sum(widened * widened, axis=1)) / D + epsilon)
    normed = (widened * norm_gain[None, :]).astype(jnp.bfloat16)

    def project(weight):
        return jnp.dot(normed, weight, preferred_element_type=jnp.float32) * row_scale[:, None]
    angles = angles_for(lengths, DH)
    query = rotate(project(query_weight).reshape(SEQS, H, 2, DH), angles).astype(jnp.bfloat16)
    fresh_key = rotate(project(key_weight).reshape(SEQS, H, 2, DH), angles).astype(jnp.bfloat16)
    fresh_value = project(value_weight).reshape(SEQS, H, 2 * DH).astype(jnp.bfloat16)

    def per_block(block_index):
        offset = block_index * POS_DEV
        positions = offset + jnp.arange(POS_DEV, dtype=jnp.int32)
        key_block = lax.dynamic_slice_in_dim(key_cache, offset, POS_DEV, 1).reshape(SEQS, POS_DEV, H, 2, DH)
        value_block = lax.dynamic_slice_in_dim(value_cache, offset, POS_DEV, 1)
        at_length = positions[None, :] == lengths[:, None]
        key_block = jnp.where(at_length[:, :, None, None, None], fresh_key[:, None], key_block)
        value_block = jnp.where(at_length[:, :, None, None], fresh_value[:, None], value_block)
        scores = jnp.einsum('shjd,sphjd->shjp', query.astype(jnp.float32), key_block.astype(jnp.float32)) * DH ** (-0.5)
        visible = (positions[None, :] <= lengths[:, None])[:, None, None, :]
        masked = jnp.where(visible, scores, floor_value)
        block_max = lax.optimization_barrier(jnp.max(masked, axis=-1))
        weights = jnp.where(visible, jnp.exp(masked - block_max[..., None]), 0.0).astype(jnp.bfloat16)
        block_total = lax.optimization_barrier(jnp.sum(weights.astype(jnp.float32), axis=-1))
        block_values = jnp.einsum('shjp,sphe->shje', weights.astype(jnp.float32), value_block.astype(jnp.float32))
        return (block_max, block_total, block_values)
    maxima, totals, valued = lax.map(per_block, jnp.arange(N_KV, dtype=jnp.int32))
    highest = lax.optimization_barrier(jnp.max(maxima, axis=0))
    factor = jnp.exp(maxima - highest[None])
    total = lax.optimization_barrier(jnp.sum(totals * factor, axis=0))
    weighted = lax.optimization_barrier(jnp.sum(valued * factor[..., None], axis=0))
    mixed_heads = weighted[:, :, 0] / total[:, :, 0, None] - lambdas[None, :, None] * weighted[:, :, 1] / total[:, :, 1, None]
    head_out = mixed_heads * lax.rsqrt(lax.optimization_barrier(jnp.mean(mixed_heads * mixed_heads, axis=-1, keepdims=True)) + epsilon) * head_gain
    head_out = head_out.astype(jnp.bfloat16).reshape(SEQS, H * 2 * DH)
    return jnp.dot(head_out, out_weight, preferred_element_type=jnp.float32).astype(jnp.bfloat16)
```

```python
import functools

import jax
import jax.numpy as jnp
import numpy as np
from jax import lax
from jax.experimental import pallas as pl
from jax.experimental.pallas import tpu as pltpu
from jax.sharding import PartitionSpec as P

DH = 64
LANES = 128
ROWS = 16
CHUNK = 1024
epsilon = 1e-05
theta_base = 500000.0
floor_value = -1e30
MESH = pl.DeviceIdType.MESH


def kernel(
    n_kv, n_tp,
    tok_h, gain_h, qw_h, kw_h, vw_h, ow_h, lam_s, hg_h, len_s, freq_h, k_h, v_h,
    out_ref,
    tok, gain, wbuf, owbuf, hg, freq, kbuf, vbuf, ids,
    part, part_in, fresh, mine, mine_in, heads, shares,
    small_sem, w_sem, k_sem, v_sem,
    s1, r1, s2, r2, s3, r3, s4, r4, s5, r5,
):
    me = lax.axis_index("kv")
    tp = lax.axis_index("tp")
    seqs = tok.shape[0]
    spk = seqs // n_kv
    width = tok.shape[1]
    hh = wbuf.shape[2] // LANES
    model = width * n_kv
    npairs = seqs // 2
    cols = kbuf.shape[1]
    pos_count = cols // hh
    base = me * pos_count
    start_pair = lax.div((me + 1) * spk + 1, 2)

    small = [
        pltpu.make_async_copy(src, dst, small_sem.at[n])
        for n, (src, dst) in enumerate(((tok_h, tok), (gain_h, gain), (freq_h, freq), (hg_h, hg)))
    ]
    weights_in = [
        pltpu.make_async_copy(src, wbuf.at[n], w_sem.at[n])
        for n, src in enumerate((qw_h, kw_h, vw_h))
    ]
    out_weight_in = pltpu.make_async_copy(ow_h, owbuf, w_sem.at[3])
    for copy in small + weights_in:
        copy.start()

    def pair_of(step):
        return lax.rem(start_pair + step, npairs)

    def cache_copies(step):
        at = pl.ds(2 * pair_of(step), 2)
        return (
            pltpu.make_async_copy(k_h.at[at], kbuf.at[pl.ds(2 * step, 2)], k_sem.at[step]),
            pltpu.make_async_copy(v_h.at[at], vbuf.at[pl.ds(2 * step, 2)], v_sem.at[step]),
        )

    for step in range(npairs):
        for copy in cache_copies(step):
            copy.start()
        if step == npairs // 2:
            out_weight_in.start()

    def kv_peer(j):
        return {"kv": lax.rem(me + j, n_kv), "tp": tp}

    def tp_peer(j):
        return {"kv": me, "tp": lax.rem(tp + j, n_tp)}

    barrier = pltpu.get_barrier_semaphore()
    for j in range(1, n_kv):
        pl.semaphore_signal(barrier, inc=1, device_id=kv_peer(j), device_id_type=MESH)
    for j in range(1, n_tp):
        pl.semaphore_signal(barrier, inc=1, device_id=tp_peer(j), device_id_type=MESH)

    column = lax.broadcasted_iota(jnp.int32, (2 * hh, cols), 1)
    row = lax.broadcasted_iota(jnp.int32, (2 * hh, cols), 0)
    same = lax.rem(column, hh) == lax.rem(row, hh)
    ids[...] = jnp.where(same, lax.div(column, hh), 1 << 30)

    for copy in small:
        copy.wait()
    turns = [
        (jnp.cos(angle), jnp.sin(angle))
        for angle in (
            jnp.full((1, LANES), len_s[me * spk + n], jnp.int32).astype(jnp.float32) * freq[...]
            for n in range(spk)
        )
    ]
    widened = tok[...].astype(jnp.float32)
    squares = jnp.sum(widened * widened, axis=1, keepdims=True)
    normed = (widened * gain[...]).astype(jnp.bfloat16)
    part[pl.ds(3 * hh, seqs, stride=ROWS), :] = jnp.broadcast_to(squares, (seqs, LANES))
    for n in range(3 * hh + 1, ROWS):
        part[pl.ds(n, seqs, stride=ROWS), :] = jnp.zeros((seqs, LANES), jnp.float32)
    for n in range(3):
        weights_in[n].wait()
        product = jnp.dot(normed, wbuf[n], preferred_element_type=jnp.float32)
        for h in range(hh):
            part[pl.ds(n * hh + h, seqs, stride=ROWS), :] = product[:, h * LANES:(h + 1) * LANES]

    pl.semaphore_wait(barrier, n_kv - 1 + n_tp - 1)

    block = spk * ROWS
    own = pl.ds(pl.multiple_of(me * block, block), block)
    sends = []
    for j in range(1, n_kv):
        peer = lax.rem(me + j, n_kv)
        copy = pltpu.make_async_remote_copy(
            part.at[pl.ds(pl.multiple_of(peer * block, block), block)], part_in.at[j - 1],
            s1.at[j - 1], r1.at[j - 1], device_id=kv_peer(j), device_id_type=MESH,
        )
        copy.start()
        sends.append(copy)
    total = part[own, :]
    for copy, j in zip(sends, range(1, n_kv)):
        copy.wait_recv()
        total = total + part_in[j - 1]

    lane = lax.broadcasted_iota(jnp.int32, (2 * hh, LANES), 1)
    low_half = lax.rem(lane, DH) < DH // 2
    for n in range(spk):
        piece = total[n * ROWS:(n + 1) * ROWS]
        scaled = piece * lax.rsqrt(piece[3 * hh:3 * hh + 1] / model + epsilon)
        turned = scaled[:2 * hh]
        other = jnp.where(
            low_half,
            -pltpu.roll(turned, LANES - DH // 2, 1),
            pltpu.roll(turned, DH // 2, 1),
        )
        turned = turned * turns[n][0] + other * turns[n][1]
        fresh[pl.ds(pl.multiple_of(me * block + n * ROWS, ROWS), ROWS), :] = jnp.concatenate(
            [turned, scaled[2 * hh:]], axis=0
        ).astype(jnp.bfloat16)
    for j in range(1, n_kv):
        copy = pltpu.make_async_remote_copy(
            fresh.at[own], fresh.at[own], s2.at[j - 1], r2.at[j - 1],
            device_id=kv_peer(j), device_id_type=MESH,
        )
        copy.start()
        sends.append(copy)
    for j in range(1, n_kv):
        source = lax.rem(me + n_kv - j, n_kv)
        there = pl.ds(pl.multiple_of(source * block, block), block)
        pltpu.make_async_remote_copy(
            fresh.at[there], fresh.at[there], s2.at[j - 1], r2.at[j - 1],
            device_id=kv_peer(j), device_id_type=MESH,
        ).wait_recv()

    lane_q = lax.broadcasted_iota(jnp.int32, (hh, LANES), 1)
    map_masks = [(lane_q < DH).astype(jnp.float32), (lane_q >= DH).astype(jnp.float32)]
    wide = lax.broadcasted_iota(jnp.int32, (2 * hh, LANES), 1)
    chunk = min(CHUNK, cols)

    def send_partial(s):
        owner = lax.div(s, spk)
        slot = lax.rem(owner - me + n_kv, n_kv) - 1
        local = lax.rem(s, spk)
        return owner, pltpu.make_async_remote_copy(
            mine.at[s], mine_in.at[slot, local], s3.at[s], r3.at[slot, local],
            device_id={"kv": owner, "tp": tp}, device_id_type=MESH,
        )

    def attend(step, carry):
        for copy in cache_copies(step):
            copy.wait()
        pair = pair_of(step)
        queries, fresh_scores, fresh_values, reach = [], [], [], []
        for u in range(2):
            s = 2 * pair + u
            rows = fresh[pl.ds(pl.multiple_of(s * ROWS, ROWS), ROWS), :].astype(jnp.float32)
            query = rows[:hh] * DH ** (-0.5)
            query = jnp.concatenate([query * map_masks[0], query * map_masks[1]], axis=0)
            keys = jnp.concatenate([rows[hh:2 * hh]] * 2, axis=0)
            reach.append(len_s[s] - base)
            inside = jnp.full((2 * hh, 1), reach[u], jnp.int32)
            inside = (inside >= 0) & (inside < pos_count)
            score = jnp.sum(query * keys, axis=1, keepdims=True)
            fresh_scores.append(jnp.where(inside, score, floor_value))
            fresh_values.append(jnp.concatenate([rows[2 * hh:3 * hh]] * 2, axis=0))
            queries.append(query.astype(jnp.bfloat16))
        none = jnp.zeros_like(queries[0])
        left = jnp.concatenate(
            [
                jnp.concatenate([queries[0], none], axis=1),
                jnp.concatenate([none, queries[1]], axis=1),
            ],
            axis=0,
        )
        masked = [[], []]
        for c in range(0, cols, chunk):
            keys = jnp.concatenate(
                [kbuf[2 * step, c:c + chunk, :], kbuf[2 * step + 1, c:c + chunk, :]], axis=1
            )
            scores = lax.dot_general(
                left, keys, (((1,), (1,)), ((), ())), preferred_element_type=jnp.float32
            )
            for u in range(2):
                masked[u].append(
                    jnp.where(
                        ids[:, c:c + chunk] < reach[u],
                        scores[u * 2 * hh:(u + 1) * 2 * hh],
                        floor_value,
                    )
                )
        tops, safe = [], []
        for u in range(2):
            joint = functools.reduce(jnp.maximum, masked[u])
            top = jnp.maximum(jnp.max(joint, axis=1, keepdims=True), fresh_scores[u])
            tops.append(top)
            safe.append(jnp.maximum(top, floor_value * 0.1))
        values = jnp.zeros((4 * hh, 2 * LANES), jnp.float32)
        sums = [None, None]
        for n, c in enumerate(range(0, cols, chunk)):
            both = []
            for u in range(2):
                weight = jnp.exp(masked[u][n] - safe[u]).astype(jnp.bfloat16)
                grown = weight.astype(jnp.float32)
                sums[u] = grown if n == 0 else sums[u] + grown
                both.append(weight)
            vals = jnp.concatenate(
                [vbuf[2 * step, c:c + chunk, :], vbuf[2 * step + 1, c:c + chunk, :]], axis=1
            )
            values = values + jnp.dot(
                jnp.concatenate(both, axis=0), vals, preferred_element_type=jnp.float32
            )
        for u in range(2):
            s = 2 * pair + u
            fresh_weight = jnp.exp(fresh_scores[u] - safe[u]).astype(jnp.bfloat16)
            fresh_weight = fresh_weight.astype(jnp.float32)
            amount = jnp.sum(sums[u], axis=1, keepdims=True) + fresh_weight
            weighted = values[u * 2 * hh:(u + 1) * 2 * hh, u * LANES:(u + 1) * LANES]
            weighted = weighted + fresh_weight * fresh_values[u]
            mine[s, :2 * hh, :] = weighted
            mine[s, 2 * hh:, :] = jnp.where(wide < DH, tops[u], amount)
            owner, copy = send_partial(s)

            @pl.when(owner != me)
            def _():
                copy.start()

        return carry

    lax.fori_loop(0, npairs, attend, 0)

    gains = hg[...]
    row_h = lax.broadcasted_iota(jnp.int32, (hh, LANES), 0)
    lambda_rows = jnp.zeros((hh, LANES), jnp.float32)
    for h in range(hh):
        lambda_rows = jnp.where(row_h == h, lam_s[h], lambda_rows)
    for n in range(spk):
        s = me * spk + n
        blocks = [mine[s]]
        for j in range(1, n_kv):
            pltpu.make_async_remote_copy(
                mine.at[s], mine_in.at[j - 1, n], s3.at[s], r3.at[j - 1, n],
                device_id=kv_peer(j), device_id_type=MESH,
            ).wait_recv()
            blocks.append(mine_in[j - 1, n])
        maxima, amounts = [], []
        for piece in blocks:
            packed = piece[2 * hh:]
            swapped = pltpu.roll(packed, DH, 1)
            maxima.append(jnp.where(wide < DH, packed, swapped))
            amounts.append(jnp.where(wide < DH, swapped, packed))
        top = functools.reduce(jnp.maximum, maxima)
        amount = jnp.zeros_like(top)
        weighted = jnp.zeros_like(top)
        for piece, biggest, sum_there in zip(blocks, maxima, amounts):
            factor = jnp.exp(biggest - top)
            amount = amount + factor * sum_there
            weighted = weighted + factor * piece[:2 * hh]
        ratio = weighted / amount
        mixed = ratio[:hh] - lambda_rows * ratio[hh:]
        mean = jnp.mean(mixed * mixed, axis=1, keepdims=True)
        head_out = mixed * lax.rsqrt(mean + epsilon) * gains
        heads[pl.ds(pl.multiple_of(s * 2 * hh, 2 * hh), 2 * hh), :] = jnp.concatenate(
            [head_out, head_out], axis=0
        )
    size = spk * 2 * hh
    own_heads = pl.ds(pl.multiple_of(me * size, size), size)
    for j in range(1, n_kv):
        copy = pltpu.make_async_remote_copy(
            heads.at[own_heads], heads.at[own_heads], s4.at[j - 1], r4.at[j - 1],
            device_id=kv_peer(j), device_id_type=MESH,
        )
        copy.start()
        sends.append(copy)
    out_weight_in.wait()
    for j in range(1, n_kv):
        source = lax.rem(me + n_kv - j, n_kv)
        there = pl.ds(pl.multiple_of(source * size, size), size)
        pltpu.make_async_remote_copy(
            heads.at[there], heads.at[there], s4.at[j - 1], r4.at[j - 1],
            device_id=kv_peer(j), device_id_type=MESH,
        ).wait_recv()
    head_row = jnp.concatenate(
        [heads[pl.ds(h, seqs, stride=2 * hh), :] for h in range(hh)], axis=1
    ).astype(jnp.bfloat16)
    share = jnp.dot(head_row, owbuf[...], preferred_element_type=jnp.float32)
    shares[tp] = share.astype(jnp.bfloat16)
    for j in range(1, n_tp):
        copy = pltpu.make_async_remote_copy(
            shares.at[tp], shares.at[tp], s5.at[j - 1], r5.at[j - 1],
            device_id=tp_peer(j), device_id_type=MESH,
        )
        copy.start()
        sends.append(copy)
    for j in range(1, n_tp):
        source = lax.rem(tp + n_tp - j, n_tp)
        pltpu.make_async_remote_copy(
            shares.at[source], shares.at[source], s5.at[j - 1], r5.at[j - 1],
            device_id=tp_peer(j), device_id_type=MESH,
        ).wait_recv()
    result = shares[0].astype(jnp.float32)
    for n in range(1, n_tp):
        result = result + shares[n].astype(jnp.float32)
    out_ref[...] = result.astype(out_ref.dtype)

    for copy in sends:
        copy.wait_send()

    def drain(step, carry):
        s = lax.rem((me + 1) * spk + step, seqs)
        _, copy = send_partial(s)
        copy.wait_send()
        return carry

    lax.fori_loop(0, seqs - spk, drain, 0)


def solution(mesh):
    n_kv, n_tp = mesh.shape["kv"], mesh.shape["tp"]

    def local(
        tokens, norm_gain, query_weight, key_weight, value_weight, out_weight,
        lambdas, head_gain, lengths, key_cache, value_cache,
    ):
        seqs, width = tokens.shape
        inner = query_weight.shape[1]
        hh = inner // LANES
        out_width = out_weight.shape[1]
        cols = key_cache.shape[1] * hh
        spk = seqs // n_kv
        flat = (seqs, cols, LANES)
        halfway = DH // 2
        frequency = np.float32(theta_base) ** (
            -(np.arange(LANES) % halfway).astype(np.float64) / halfway
        )
        frequency = jnp.asarray(frequency.astype(np.float32)[None, :])
        whole = pl.BlockSpec(memory_space=pl.ANY)
        scalars = pl.BlockSpec(memory_space=pltpu.SMEM)
        dma = pltpu.SemaphoreType.DMA
        return pl.pallas_call(
            functools.partial(kernel, n_kv, n_tp),
            out_shape=jax.ShapeDtypeStruct((seqs, out_width), jnp.bfloat16),
            in_specs=[whole] * 6 + [scalars, whole, scalars] + [whole] * 3,
            out_specs=pl.BlockSpec(memory_space=pltpu.VMEM),
            scratch_shapes=[
                pltpu.VMEM((seqs, width), jnp.bfloat16),
                pltpu.VMEM((1, width), jnp.float32),
                pltpu.VMEM((3, width, inner), jnp.bfloat16),
                pltpu.VMEM((inner, out_width), jnp.bfloat16),
                pltpu.VMEM((1, LANES), jnp.float32),
                pltpu.VMEM((1, LANES), jnp.float32),
                pltpu.VMEM(flat, jnp.bfloat16),
                pltpu.VMEM(flat, jnp.bfloat16),
                pltpu.VMEM((2 * hh, cols), jnp.int32),
                pltpu.VMEM((seqs * ROWS, LANES), jnp.float32),
                pltpu.VMEM((n_kv - 1, spk * ROWS, LANES), jnp.float32),
                pltpu.VMEM((seqs * ROWS, LANES), jnp.bfloat16),
                pltpu.VMEM((seqs, 4 * hh, LANES), jnp.float32),
                pltpu.VMEM((n_kv - 1, spk, 4 * hh, LANES), jnp.float32),
                pltpu.VMEM((seqs * 2 * hh, LANES), jnp.float32),
                pltpu.VMEM((n_tp, seqs, out_width), jnp.bfloat16),
                dma((4,)), dma((4,)), dma((seqs // 2,)), dma((seqs // 2,)),
                dma((n_kv - 1,)), dma((n_kv - 1,)),
                dma((n_kv - 1,)), dma((n_kv - 1,)),
                dma((seqs,)), dma((n_kv - 1, spk)),
                dma((n_kv - 1,)), dma((n_kv - 1,)),
                dma((n_tp - 1,)), dma((n_tp - 1,)),
            ],
            compiler_params=pltpu.CompilerParams(
                collective_id=0, has_side_effects=True, vmem_limit_bytes=60 * 1024 * 1024
            ),
        )(
            tokens, norm_gain.reshape(1, width), query_weight, key_weight, value_weight,
            out_weight, lambdas, head_gain.reshape(1, LANES), lengths, frequency,
            key_cache.reshape(flat), value_cache.reshape(flat),
        )

    return jax.shard_map(
        local,
        mesh=mesh,
        in_specs=(
            P(None, "kv"), P("kv"), P("kv", "tp"), P("kv", "tp"), P("kv", "tp"), P("tp", "kv"),
            P("tp"), P(), P(), P(None, "kv", "tp", None), P(None, "kv", "tp", None),
        ),
        out_specs=P(None, "kv"),
        check_vma=False,
    )
```

```python
import functools

import jax
import jax.numpy as jnp
import numpy as np
from jax import lax
from jax.experimental import pallas as pl
from jax.experimental.pallas import tpu as pltpu
from jax.sharding import PartitionSpec as P

DH = 64
LANES = 128
ROWS = 16
CHUNK = 1024
epsilon = 1e-05
theta_base = 500000.0
floor_value = -1e30
MESH = pl.DeviceIdType.MESH


def kernel(
    n_kv, n_tp,
    tok_h, gain_h, qw_h, kw_h, vw_h, ow_h, lam_s, hg_h, len_s, freq_h, k_h, v_h,
    out_ref,
    tok, gain, wbuf, owbuf, hg, freq, kbuf, vbuf, ids,
    part, part_in, fresh, mine, mine_in, heads, shares,
    small_sem, w_sem, k_sem, v_sem,
    s1, r1, s2, r2, s3, r3, s4, r4, s5, r5,
):
    me = lax.axis_index("kv")
    tp = lax.axis_index("tp")
    seqs = tok.shape[0]
    spk = seqs // n_kv
    width = tok.shape[1]
    hh = wbuf.shape[2] // LANES
    model = width * n_kv
    npairs = seqs // 2
    cols = kbuf.shape[1]
    pos_count = cols // hh
    base = me * pos_count
    start_pair = lax.div((me + 1) * spk + 1, 2)

    def kv_peer(j):
        return {"kv": lax.rem(me + j, n_kv), "tp": tp}

    def tp_peer(j):
        return {"kv": me, "tp": lax.rem(tp + j, n_tp)}

    barrier = pltpu.get_barrier_semaphore()
    for j in range(1, n_kv):
        pl.semaphore_signal(barrier, inc=1, device_id=kv_peer(j), device_id_type=MESH)
    for j in range(1, n_tp):
        pl.semaphore_signal(barrier, inc=1, device_id=tp_peer(j), device_id_type=MESH)

    small = [
        pltpu.make_async_copy(src, dst, small_sem.at[n])
        for n, (src, dst) in enumerate(((tok_h, tok), (gain_h, gain), (freq_h, freq), (hg_h, hg)))
    ]
    weights_in = [
        pltpu.make_async_copy(src, wbuf.at[n], w_sem.at[n])
        for n, src in enumerate((qw_h, kw_h, vw_h))
    ]
    out_weight_in = pltpu.make_async_copy(ow_h, owbuf, w_sem.at[3])
    for copy in small + weights_in:
        copy.start()

    def pair_of(step):
        return lax.rem(start_pair + step, npairs)

    def cache_copies(step):
        at = pl.ds(2 * pair_of(step), 2)
        return (
            pltpu.make_async_copy(k_h.at[at], kbuf.at[pl.ds(2 * step, 2)], k_sem.at[step]),
            pltpu.make_async_copy(v_h.at[at], vbuf.at[pl.ds(2 * step, 2)], v_sem.at[step]),
        )


    column = lax.broadcasted_iota(jnp.int32, (2 * hh, cols), 1)
    row = lax.broadcasted_iota(jnp.int32, (2 * hh, cols), 0)
    same = lax.rem(column, hh) == lax.rem(row, hh)
    ids[...] = jnp.where(same, lax.div(column, hh), 1 << 30)

    for copy in small:
        copy.wait()
    turns = [
        (jnp.cos(angle), jnp.sin(angle))
        for angle in (
            jnp.full((1, LANES), len_s[me * spk + n], jnp.int32).astype(jnp.float32) * freq[...]
            for n in range(spk)
        )
    ]
    widened = tok[...].astype(jnp.float32)
    squares = jnp.sum(widened * widened, axis=1, keepdims=True)
    normed = (widened * gain[...]).astype(jnp.bfloat16)
    part[pl.ds(3 * hh, seqs, stride=ROWS), :] = jnp.broadcast_to(squares, (seqs, LANES))
    for n in range(3 * hh + 1, ROWS):
        part[pl.ds(n, seqs, stride=ROWS), :] = jnp.zeros((seqs, LANES), jnp.float32)
    for n in range(3):
        weights_in[n].wait()
        product = jnp.dot(normed, wbuf[n], preferred_element_type=jnp.float32)
        for h in range(hh):
            part[pl.ds(n * hh + h, seqs, stride=ROWS), :] = product[:, h * LANES:(h + 1) * LANES]

    for step in range(npairs):
        for copy in cache_copies(step):
            copy.start()
        if step == npairs // 2:
            out_weight_in.start()
    pl.semaphore_wait(barrier, n_kv - 1 + n_tp - 1)

    block = spk * ROWS
    own = pl.ds(pl.multiple_of(me * block, block), block)
    sends = []
    for j in range(1, n_kv):
        peer = lax.rem(me + j, n_kv)
        copy = pltpu.make_async_remote_copy(
            part.at[pl.ds(pl.multiple_of(peer * block, block), block)], part_in.at[j - 1],
            s1.at[j - 1], r1.at[j - 1], device_id=kv_peer(j), device_id_type=MESH,
        )
        copy.start()
        sends.append(copy)
    total = part[own, :]
    for copy, j in zip(sends, range(1, n_kv)):
        copy.wait_recv()
        total = total + part_in[j - 1]

    lane = lax.broadcasted_iota(jnp.int32, (2 * hh, LANES), 1)
    low_half = lax.rem(lane, DH) < DH // 2
    for n in range(spk):
        piece = total[n * ROWS:(n + 1) * ROWS]
        scaled = piece * lax.rsqrt(piece[3 * hh:3 * hh + 1] / model + epsilon)
        turned = scaled[:2 * hh]
        other = jnp.where(
            low_half,
            -pltpu.roll(turned, LANES - DH // 2, 1),
            pltpu.roll(turned, DH // 2, 1),
        )
        turned = turned * turns[n][0] + other * turns[n][1]
        fresh[pl.ds(pl.multiple_of(me * block + n * ROWS, ROWS), ROWS), :] = jnp.concatenate(
            [turned, scaled[2 * hh:]], axis=0
        ).astype(jnp.bfloat16)
    for j in range(1, n_kv):
        copy = pltpu.make_async_remote_copy(
            fresh.at[own], fresh.at[own], s2.at[j - 1], r2.at[j - 1],
            device_id=kv_peer(j), device_id_type=MESH,
        )
        copy.start()
        sends.append(copy)
    for j in range(1, n_kv):
        source = lax.rem(me + n_kv - j, n_kv)
        there = pl.ds(pl.multiple_of(source * block, block), block)
        pltpu.make_async_remote_copy(
            fresh.at[there], fresh.at[there], s2.at[j - 1], r2.at[j - 1],
            device_id=kv_peer(j), device_id_type=MESH,
        ).wait_recv()

    lane_q = lax.broadcasted_iota(jnp.int32, (hh, LANES), 1)
    map_masks = [(lane_q < DH).astype(jnp.float32), (lane_q >= DH).astype(jnp.float32)]
    wide = lax.broadcasted_iota(jnp.int32, (2 * hh, LANES), 1)
    chunk = min(CHUNK, cols)

    def send_partial(s):
        owner = lax.div(s, spk)
        slot = lax.rem(owner - me + n_kv, n_kv) - 1
        local = lax.rem(s, spk)
        return owner, pltpu.make_async_remote_copy(
            mine.at[s], mine_in.at[slot, local], s3.at[s], r3.at[slot, local],
            device_id={"kv": owner, "tp": tp}, device_id_type=MESH,
        )

    def attend(step, carry):
        for copy in cache_copies(step):
            copy.wait()
        pair = pair_of(step)
        queries, fresh_scores, fresh_values, reach = [], [], [], []
        for u in range(2):
            s = 2 * pair + u
            rows = fresh[pl.ds(pl.multiple_of(s * ROWS, ROWS), ROWS), :].astype(jnp.float32)
            query = rows[:hh] * DH ** (-0.5)
            query = jnp.concatenate([query * map_masks[0], query * map_masks[1]], axis=0)
            keys = jnp.concatenate([rows[hh:2 * hh]] * 2, axis=0)
            reach.append(len_s[s] - base)
            inside = jnp.full((2 * hh, 1), reach[u], jnp.int32)
            inside = (inside >= 0) & (inside < pos_count)
            score = jnp.sum(query * keys, axis=1, keepdims=True)
            fresh_scores.append(jnp.where(inside, score, floor_value))
            fresh_values.append(jnp.concatenate([rows[2 * hh:3 * hh]] * 2, axis=0))
            queries.append(query.astype(jnp.bfloat16))
        none = jnp.zeros_like(queries[0])
        left = jnp.concatenate(
            [
                jnp.concatenate([queries[0], none], axis=1),
                jnp.concatenate([none, queries[1]], axis=1),
            ],
            axis=0,
        )
        masked = [[], []]
        for c in range(0, cols, chunk):
            keys = jnp.concatenate(
                [kbuf[2 * step, c:c + chunk, :], kbuf[2 * step + 1, c:c + chunk, :]], axis=1
            )
            scores = lax.dot_general(
                left, keys, (((1,), (1,)), ((), ())), preferred_element_type=jnp.float32
            )
            for u in range(2):
                masked[u].append(
                    jnp.where(
                        ids[:, c:c + chunk] < reach[u],
                        scores[u * 2 * hh:(u + 1) * 2 * hh],
                        floor_value,
                    )
                )
        tops, safe = [], []
        for u in range(2):
            joint = functools.reduce(jnp.maximum, masked[u])
            top = jnp.maximum(jnp.max(joint, axis=1, keepdims=True), fresh_scores[u])
            tops.append(top)
            safe.append(jnp.maximum(top, floor_value * 0.1))
        values = jnp.zeros((4 * hh, 2 * LANES), jnp.float32)
        sums = [None, None]
        for n, c in enumerate(range(0, cols, chunk)):
            both = []
            for u in range(2):
                weight = jnp.exp(masked[u][n] - safe[u]).astype(jnp.bfloat16)
                grown = weight.astype(jnp.float32)
                sums[u] = grown if n == 0 else sums[u] + grown
                both.append(weight)
            vals = jnp.concatenate(
                [vbuf[2 * step, c:c + chunk, :], vbuf[2 * step + 1, c:c + chunk, :]], axis=1
            )
            values = values + jnp.dot(
                jnp.concatenate(both, axis=0), vals, preferred_element_type=jnp.float32
            )
        for u in range(2):
            s = 2 * pair + u
            fresh_weight = jnp.exp(fresh_scores[u] - safe[u]).astype(jnp.bfloat16)
            fresh_weight = fresh_weight.astype(jnp.float32)
            amount = jnp.sum(sums[u], axis=1, keepdims=True) + fresh_weight
            weighted = values[u * 2 * hh:(u + 1) * 2 * hh, u * LANES:(u + 1) * LANES]
            weighted = weighted + fresh_weight * fresh_values[u]
            mine[s, :2 * hh, :] = weighted
            mine[s, 2 * hh:, :] = jnp.where(wide < DH, tops[u], amount)
            owner, copy = send_partial(s)

            @pl.when(owner != me)
            def _():
                copy.start()

        return carry

    lax.fori_loop(0, npairs, attend, 0)

    gains = hg[...]
    row_h = lax.broadcasted_iota(jnp.int32, (hh, LANES), 0)
    lambda_rows = jnp.zeros((hh, LANES), jnp.float32)
    for h in range(hh):
        lambda_rows = jnp.where(row_h == h, lam_s[h], lambda_rows)
    for n in range(spk):
        s = me * spk + n
        blocks = [mine[s]]
        for j in range(1, n_kv):
            pltpu.make_async_remote_copy(
                mine.at[s], mine_in.at[j - 1, n], s3.at[s], r3.at[j - 1, n],
                device_id=kv_peer(j), device_id_type=MESH,
            ).wait_recv()
            blocks.append(mine_in[j - 1, n])
        maxima, amounts = [], []
        for piece in blocks:
            packed = piece[2 * hh:]
            swapped = pltpu.roll(packed, DH, 1)
            maxima.append(jnp.where(wide < DH, packed, swapped))
            amounts.append(jnp.where(wide < DH, swapped, packed))
        top = functools.reduce(jnp.maximum, maxima)
        amount = jnp.zeros_like(top)
        weighted = jnp.zeros_like(top)
        for piece, biggest, sum_there in zip(blocks, maxima, amounts):
            factor = jnp.exp(biggest - top)
            amount = amount + factor * sum_there
            weighted = weighted + factor * piece[:2 * hh]
        ratio = weighted / amount
        mixed = ratio[:hh] - lambda_rows * ratio[hh:]
        mean = jnp.mean(mixed * mixed, axis=1, keepdims=True)
        head_out = mixed * lax.rsqrt(mean + epsilon) * gains
        heads[pl.ds(pl.multiple_of(s * 2 * hh, 2 * hh), 2 * hh), :] = jnp.concatenate(
            [head_out, head_out], axis=0
        )
    size = spk * 2 * hh
    own_heads = pl.ds(pl.multiple_of(me * size, size), size)
    for j in range(1, n_kv):
        copy = pltpu.make_async_remote_copy(
            heads.at[own_heads], heads.at[own_heads], s4.at[j - 1], r4.at[j - 1],
            device_id=kv_peer(j), device_id_type=MESH,
        )
        copy.start()
        sends.append(copy)
    out_weight_in.wait()
    for j in range(1, n_kv):
        source = lax.rem(me + n_kv - j, n_kv)
        there = pl.ds(pl.multiple_of(source * size, size), size)
        pltpu.make_async_remote_copy(
            heads.at[there], heads.at[there], s4.at[j - 1], r4.at[j - 1],
            device_id=kv_peer(j), device_id_type=MESH,
        ).wait_recv()
    head_row = jnp.concatenate(
        [heads[pl.ds(h, seqs, stride=2 * hh), :] for h in range(hh)], axis=1
    ).astype(jnp.bfloat16)
    share = jnp.dot(head_row, owbuf[...], preferred_element_type=jnp.float32)
    shares[tp] = share.astype(jnp.bfloat16)
    for j in range(1, n_tp):
        copy = pltpu.make_async_remote_copy(
            shares.at[tp], shares.at[tp], s5.at[j - 1], r5.at[j - 1],
            device_id=tp_peer(j), device_id_type=MESH,
        )
        copy.start()
        sends.append(copy)
    for j in range(1, n_tp):
        source = lax.rem(tp + n_tp - j, n_tp)
        pltpu.make_async_remote_copy(
            shares.at[source], shares.at[source], s5.at[j - 1], r5.at[j - 1],
            device_id=tp_peer(j), device_id_type=MESH,
        ).wait_recv()
    result = shares[0].astype(jnp.float32)
    for n in range(1, n_tp):
        result = result + shares[n].astype(jnp.float32)
    out_ref[...] = result.astype(out_ref.dtype)

    for copy in sends:
        copy.wait_send()

    def drain(step, carry):
        s = lax.rem((me + 1) * spk + step, seqs)
        _, copy = send_partial(s)
        copy.wait_send()
        return carry

    lax.fori_loop(0, seqs - spk, drain, 0)


def solution(mesh):
    n_kv, n_tp = mesh.shape["kv"], mesh.shape["tp"]

    def local(
        tokens, norm_gain, query_weight, key_weight, value_weight, out_weight,
        lambdas, head_gain, lengths, key_cache, value_cache,
    ):
        seqs, width = tokens.shape
        inner = query_weight.shape[1]
        hh = inner // LANES
        out_width = out_weight.shape[1]
        cols = key_cache.shape[1] * hh
        spk = seqs // n_kv
        flat = (seqs, cols, LANES)
        halfway = DH // 2
        frequency = np.float32(theta_base) ** (
            -(np.arange(LANES) % halfway).astype(np.float64) / halfway
        )
        frequency = jnp.asarray(frequency.astype(np.float32)[None, :])
        whole = pl.BlockSpec(memory_space=pl.ANY)
        scalars = pl.BlockSpec(memory_space=pltpu.SMEM)
        dma = pltpu.SemaphoreType.DMA
        return pl.pallas_call(
            functools.partial(kernel, n_kv, n_tp),
            out_shape=jax.ShapeDtypeStruct((seqs, out_width), jnp.bfloat16),
            in_specs=[whole] * 6 + [scalars, whole, scalars] + [whole] * 3,
            out_specs=pl.BlockSpec(memory_space=pltpu.VMEM),
            scratch_shapes=[
                pltpu.VMEM((seqs, width), jnp.bfloat16),
                pltpu.VMEM((1, width), jnp.float32),
                pltpu.VMEM((3, width, inner), jnp.bfloat16),
                pltpu.VMEM((inner, out_width), jnp.bfloat16),
                pltpu.VMEM((1, LANES), jnp.float32),
                pltpu.VMEM((1, LANES), jnp.float32),
                pltpu.VMEM(flat, jnp.bfloat16),
                pltpu.VMEM(flat, jnp.bfloat16),
                pltpu.VMEM((2 * hh, cols), jnp.int32),
                pltpu.VMEM((seqs * ROWS, LANES), jnp.float32),
                pltpu.VMEM((n_kv - 1, spk * ROWS, LANES), jnp.float32),
                pltpu.VMEM((seqs * ROWS, LANES), jnp.bfloat16),
                pltpu.VMEM((seqs, 4 * hh, LANES), jnp.float32),
                pltpu.VMEM((n_kv - 1, spk, 4 * hh, LANES), jnp.float32),
                pltpu.VMEM((seqs * 2 * hh, LANES), jnp.float32),
                pltpu.VMEM((n_tp, seqs, out_width), jnp.bfloat16),
                dma((4,)), dma((4,)), dma((seqs // 2,)), dma((seqs // 2,)),
                dma((n_kv - 1,)), dma((n_kv - 1,)),
                dma((n_kv - 1,)), dma((n_kv - 1,)),
                dma((seqs,)), dma((n_kv - 1, spk)),
                dma((n_kv - 1,)), dma((n_kv - 1,)),
                dma((n_tp - 1,)), dma((n_tp - 1,)),
            ],
            compiler_params=pltpu.CompilerParams(
                collective_id=0, has_side_effects=True, vmem_limit_bytes=60 * 1024 * 1024
            ),
        )(
            tokens, norm_gain.reshape(1, width), query_weight, key_weight, value_weight,
            out_weight, lambdas, head_gain.reshape(1, LANES), lengths, frequency,
            key_cache.reshape(flat), value_cache.reshape(flat),
        )

    return jax.shard_map(
        local,
        mesh=mesh,
        in_specs=(
            P(None, "kv"), P("kv"), P("kv", "tp"), P("kv", "tp"), P("kv", "tp"), P("tp", "kv"),
            P("tp"), P(), P(), P(None, "kv", "tp", None), P(None, "kv", "tp", None),
        ),
        out_specs=P(None, "kv"),
        check_vma=False,
    )
```
